32 devices in a mesh: fs: 8 (over z, x), tp: 4 (over y, core).
Axes of the slice: x: 2, y: 2, z: 4, core: 2. Of those that a mesh axis runs over, the one named last changes fastest.
Arguments:
- tokens: bfloat16 [8192, 2048], P(('fs', 'tp')), may hold values from -130 to 130
- pool_weight: bfloat16 [4, 512, 512], P(None, 'fs'), may hold values from -0.25 to 0.25
- pool_scale: float32 [2048], replicated, may hold values from 0.5 to 1.5
- gain_mix: float32 [2048], replicated, may hold values from 0.1 to 1.9
- gain_mlp: float32 [2048], replicated, may hold values from 0.1 to 1.9
- w_up: bfloat16 [8192, 2048], P('tp', 'fs'), may hold values from -0.125 to 0.125
- w_down: bfloat16 [8192, 2048], P('tp', 'fs'), may hold values from -0.0625 to 0.0625
- gain_out: float32 [2048], P('tp'), may hold values from 0.1 to 1.9
Outputs:
- result: bfloat16 [8192, 2048], P('fs', 'tp')
The draws below stay inside these ranges and needn't reach their ends.
All inputs are finite; a program needn't handle non-finite values.
Results may differ from the reference program's by a relative error of at most 0.013.
Values may be sent and summed in bfloat16 or wider, within the bound.
A program may use at most 64 MiB of HBM per device.

```python
import math
import jax
import jax.numpy as jnp
from jax import lax

D = 2048
FF = 8192
GROUP = 512
SEQ_LEN = 1024
TOKENS = 8192
N_TP = 4


def draw_tokens(key, part):
    key_row, key_col, key_base = jax.random.split(jax.random.fold_in(key, 11), 3)
    column = jnp.arange(D, dtype=jnp.float32) / D
    row_scale = jnp.exp(jax.random.uniform(key_row, (TOKENS, 1), jnp.float32, math.log(0.5), math.log(5.0)))
    col_scale = jnp.exp(jax.random.uniform(key_col, (1, D), jnp.float32, math.log(0.4), math.log(2.5)))
    base = jnp.clip(jax.random.normal(key_base, (TOKENS, D), jnp.float32), -4.0, 4.0)
    trend = 3.0 ** (0.5 * column)
    return (base * row_scale * col_scale * trend[None, :]).astype(jnp.bfloat16)


def steps_of(key, dims, shards, least, largest):
    factor_of, own = 1.0, jax.random.fold_in(key, 6)
    for dim, shards_of in shards:
        heights = jnp.exp(jax.random.uniform(jax.random.fold_in(own, dim), (shards_of,), jnp.float32, least / len(shards), largest / len(shards)))
        factor_of = factor_of * jnp.repeat(heights, dims[dim] // shards_of).reshape([-1 if axis == dim else 1 for axis in range(len(dims))])
    return factor_of


def centred(stream_key, extent, spread, most, cuts=(), kind=jnp.bfloat16):
    level = steps_of(stream_key, extent, cuts, -0.22, 0.18) if cuts else 1.0
    drawn = jax.random.normal(stream_key, extent, jnp.float32) * spread * level
    return jnp.minimum(jnp.maximum(drawn, -most), most).astype(kind)


def setup_inputs(seed: int = 0) -> dict:
    arg_keys = jax.random.split(jax.random.key(seed), 9)
    tokens = draw_tokens(jax.random.fold_in(arg_keys[8], 71), 0)
    pool_weight = centred(arg_keys[1], (4, GROUP, GROUP), GROUP ** -0.5, 0.25, ((1, 8),))
    pool_scale = jnp.clip(jax.random.uniform(arg_keys[2], (D,), jnp.float32, 0.5, 1.5), 0.5, 1.5)
    gain_mix = jnp.clip(1.0 + 0.18 * jax.random.normal(arg_keys[3], (D,), jnp.float32), 0.1, 1.9)
    gain_mlp = jnp.clip(1.0 + 0.18 * jax.random.normal(arg_keys[4], (D,), jnp.float32), 0.1, 1.9)
    w_up = centred(arg_keys[5], (FF, D), D ** -0.5, 0.125, ((0, 4), (1, 8)))
    w_down = centred(arg_keys[6], (FF, D), FF ** -0.5, 0.0625, ((0, 4), (1, 8)))
    gain_out = jnp.clip(1.0 + 0.18 * jax.random.normal(arg_keys[7], (D,), jnp.float32), 0.1, 1.9)
    return dict(tokens=tokens, pool_weight=pool_weight, pool_scale=pool_scale, gain_mix=gain_mix, gain_mlp=gain_mlp, w_up=w_up, w_down=w_down, gain_out=gain_out)


EPS = 1e-06
WINDOWS = (2, 4, 8, 16)

def rms_scale(values, gain):
    return values * lax.rsqrt(lax.optimization_barrier(jnp.mean(values * values, axis=-1, keepdims=True)) + EPS) * gain

def window_mean(values, reach):
    cumulative = jnp.concatenate([jnp.zeros_like(values[:, :1]), jnp.cumsum(values, axis=1)], axis=1)
    position = jnp.arange(SEQ_LEN, dtype=jnp.int32)
    lower = jnp.clip(position - reach // 2, 0, SEQ_LEN).astype(jnp.int32)
    upper = jnp.clip(position + reach // 2, 0, SEQ_LEN).astype(jnp.int32)
    sums = jnp.take(cumulative, upper, axis=1) - jnp.take(cumulative, lower, axis=1)
    counts = (upper - lower).astype(jnp.float32)[None, :, None]
    return sums / counts

def reference(tokens, pool_weight, pool_scale, gain_mix, gain_mlp, w_up, w_down, gain_out):
    inputs = tokens.astype(jnp.float32)
    normed = rms_scale(inputs, gain_mix).astype(jnp.bfloat16)
    normed_seq = normed.astype(jnp.float32).reshape(-1, SEQ_LEN, D)
    pieces = []
    for index, reach in enumerate(WINDOWS):
        part = normed_seq[..., index * GROUP:(index + 1) * GROUP]
        pooled = (window_mean(part, reach) - part).astype(jnp.bfloat16).reshape(-1, GROUP)
        pieces.append(jnp.dot(pooled, pool_weight[index], preferred_element_type=jnp.float32))
    mixed = jnp.concatenate(pieces, axis=1) * pool_scale
    first_sum = (inputs + mixed).astype(jnp.bfloat16)
    first_f32 = first_sum.astype(jnp.float32)
    inner = rms_scale(first_f32, gain_mlp).astype(jnp.bfloat16)
    block = FF // N_TP

    def add_block(index, total):
        begin = (index * block).astype(jnp.int32)
        up_block = lax.dynamic_slice_in_dim(w_up, begin, block, 0)
        down_block = lax.dynamic_slice_in_dim(w_down, begin, block, 0)
        pre = jnp.dot(inner, up_block.T, preferred_element_type=jnp.float32)
        hidden = jnp.square(jax.nn.relu(pre)).astype(jnp.bfloat16)
        partial_sum = jnp.dot(hidden, down_block, preferred_element_type=jnp.float32).astype(jnp.bfloat16)
        partial_sum = lax.optimization_barrier(partial_sum)
        return total + partial_sum.astype(jnp.float32)
    channel_out = lax.fori_loop(jnp.int32(0), jnp.int32(N_TP), add_block, jnp.zeros((tokens.shape[0], D), jnp.float32))
    second_sum = first_f32 + channel_out
    return rms_scale(second_sum, gain_out).astype(jnp.bfloat16)
```

```python
import functools

import jax
import jax.numpy as jnp
from jax import lax
from jax.experimental import pallas as pl
from jax.experimental.pallas import tpu as pltpu
from jax.sharding import PartitionSpec as P

SEQ_LEN = 1024
EPS = 1e-06
WINDOWS = (2, 4, 8, 16)
HALO = 16
MESH = pl.DeviceIdType.MESH
POOL, UP, DOWN = 0, 1, 2


def ring_order(n, nx):
    nz = n // nx
    if nx < 2 or nz < 2 or nz % 2:
        return list(range(n))
    order = []
    for z in range(nz):
        xs = list(range(1, nx))
        order += [z * nx + x for x in (xs if z % 2 == 0 else xs[::-1])]
    return order + [z * nx for z in range(nz - 1, -1, -1)]


def lookup(table, index):
    value = jnp.int32(table[0])
    for i in range(1, len(table)):
        value = jnp.where(index == i, jnp.int32(table[i]), value)
    return value


def kernel(
    n, tp, order, tok_ref, pool_ref, up_ref, down_ref, scale_ref, gmix_ref, gmlp_ref, out_ref,
    pool_full, up_full, down_full, ext, first, inner_all, hidden, fcols, blocks, parts,
    before, after, edge,
    ring_send, ring_recv, in_send, in_recv, fc_send, fc_recv, halo_send, halo_recv, rs_send, rs_recv,
):
    rows, width = tok_ref.shape
    group = width // 4
    hid, cols = up_ref.shape
    depth = pool_ref.shape[1]
    own_cols = width // tp
    per = n // tp
    seq = rows * tp
    me_fs, me = lax.axis_index("fs"), lax.axis_index("tp")
    place_of = [order.index(i) for i in range(n)]
    place = lookup(place_of, me_fs)

    def at(offset):
        return lookup(order, lax.rem(place + offset + 2 * n, n))

    owners = {0: me_fs}
    for d in range(1, n // 2 + 1):
        owners[d] = at(d)
        owners[-d] = at(-d)
    right, left = owners[1], owners[-1]

    barrier = pltpu.get_barrier_semaphore()
    for peer in (right, left):
        pl.semaphore_signal(barrier, inc=1, device_id={"fs": peer, "tp": me}, device_id_type=MESH)
    for d in range(1, tp):
        pl.semaphore_signal(
            barrier, inc=1, device_id={"fs": me_fs, "tp": lax.rem(me + d, tp)}, device_id_type=MESH
        )
    pl.semaphore_wait(barrier, 2 + tp - 1)

    hops = n // 2

    def view(stream, full, owner, piece):
        if stream == POOL:
            ref = pool_full if full else pool_ref
            half = ref.shape[0] // 2
            r = pl.ds(pl.multiple_of(owner * depth, depth), depth) if full else slice(None)
            return ref.at[pl.ds(piece * half, half), r, :]
        ref = (up_full if full else up_ref) if stream == UP else (down_full if full else down_ref)
        half = hid // 2
        c = pl.ds(pl.multiple_of(owner * cols, cols), cols) if full else slice(None)
        return ref.at[pl.ds(piece * half, half), c]

    def count(side, piece):
        return hops if piece == side else hops - 1

    def ring(stream, side, piece, hop):
        owner = owners[-hop] if side == 0 else owners[hop]
        return pltpu.make_async_remote_copy(
            src_ref=view(stream, hop > 0, owner, piece),
            dst_ref=view(stream, True, owner, piece),
            send_sem=ring_send.at[((stream * 2 + side) * 2 + piece) * hops + hop],
            recv_sem=ring_recv.at[((stream * 2 + side) * 2 + piece) * hops + hop],
            device_id={"fs": right if side == 0 else left, "tp": me},
            device_id_type=MESH,
        )

    started = []

    def arrived(stream, side, piece, hop):
        owner = owners[-hop - 1] if side == 0 else owners[hop + 1]
        pltpu.make_async_remote_copy(
            src_ref=view(stream, True, owner, piece),
            dst_ref=view(stream, True, owner, piece),
            send_sem=ring_send.at[((stream * 2 + side) * 2 + piece) * hops + hop],
            recv_sem=ring_recv.at[((stream * 2 + side) * 2 + piece) * hops + hop],
            device_id={"fs": right if side == 0 else left, "tp": me},
            device_id_type=MESH,
        ).wait_recv()

    def start(stream, hop, which=(0, 1)):
        for w in which:
            for side in (0, 1):
                piece = side if w == 0 else 1 - side
                if hop < count(side, piece):
                    if hop > 0:
                        arrived(stream, side, piece, hop - 1)
                    copy = ring(stream, side, piece, hop)
                    copy.start()
                    started.append(copy)

    def finish(stream):
        for side in (0, 1):
            piece = side
            arrived(stream, side, piece, hops - 1)

    def settle(stream, hop):
        if hop == hops - 2:
            for side in (0, 1):
                arrived(stream, side, 1 - side, hop)

    start(POOL, 0)
    start(UP, 0, (0,))

    step = 32 if rows % 32 == 0 else rows

    @pl.loop(0, rows // step)
    def _(i):
        r = pl.ds(pl.multiple_of(i * step, step), step)
        x = tok_ref[r, :].astype(jnp.float32)
        y = x * lax.rsqrt(jnp.mean(x * x, axis=-1, keepdims=True) + EPS) * gmix_ref[...]
        y = y.astype(jnp.bfloat16)
        ext[pl.ds(pl.multiple_of(HALO + i * step, HALO), step), :] = y.astype(jnp.float32)

    edge[0] = ext[rows : rows + HALO, :].astype(jnp.bfloat16)
    edge[1] = ext[HALO : 2 * HALO, :].astype(jnp.bfloat16)
    halos = []
    for side, (buffer, d) in enumerate(((before, 1), (after, tp - 1))):
        copy = pltpu.make_async_remote_copy(
            src_ref=edge.at[side],
            dst_ref=buffer,
            send_sem=halo_send.at[side],
            recv_sem=halo_recv.at[side],
            device_id={"fs": me_fs, "tp": lax.rem(me + d, tp)},
            device_id_type=MESH,
        )
        copy.start()
        halos.append(copy)

    start(POOL, 1)
    start(UP, 0, (1,))
    for hop in range(2, hops):
        start(POOL, hop)
    pool_full[:, pl.ds(pl.multiple_of(me_fs * depth, depth), depth), :] = pool_ref[...]
    mine = pl.ds(pl.multiple_of(me_fs * cols, cols), cols)
    up_full[:, mine] = up_ref[...]
    down_full[:, mine] = down_ref[...]
    for copy in halos:
        copy.wait()
    offset = me * rows
    lower_open = (lax.rem(offset, SEQ_LEN) != 0).astype(jnp.float32)
    upper_open = (lax.rem(offset + rows, SEQ_LEN) != 0).astype(jnp.float32)
    ext[0:HALO, :] = before[...].astype(jnp.float32) * lower_open
    ext[rows + HALO : rows + 2 * HALO, :] = after[...].astype(jnp.float32) * upper_open
    start(UP, 1)
    settle(POOL, hops - 2)
    finish(POOL)

    position = lax.rem(offset + lax.broadcasted_iota(jnp.int32, (rows, 1), 0), SEQ_LEN)
    for index, reach in enumerate(WINDOWS):
        half = reach // 2
        c = slice(index * group, (index + 1) * group)
        level = ext[:, c]
        own = level[HALO : HALO + rows]
        shift = 1
        while shift < reach:
            level = level + pltpu.roll(level, shift, 0)
            shift *= 2
        if half > 1:
            level = pltpu.roll(level, rows + 2 * HALO - (half - 1), 0)
        window = level[HALO : HALO + rows]
        counts = (jnp.minimum(position + half, SEQ_LEN) - jnp.maximum(position - half, 0)).astype(jnp.float32)
        pooled = (window / counts - own).astype(jnp.bfloat16)
        mixed = jnp.dot(pooled, pool_full[index], preferred_element_type=jnp.float32)
        first[:, c] = (tok_ref[:, c].astype(jnp.float32) + mixed * scale_ref[:, c]).astype(jnp.bfloat16)
    for hop in range(2, 3):
        if hop < hops:
            start(UP, hop)

    @pl.loop(0, rows // step)
    def _(i):
        r = pl.ds(pl.multiple_of(i * step, step), step)
        x = first[r, :].astype(jnp.float32)
        y = x * lax.rsqrt(jnp.mean(x * x, axis=-1, keepdims=True) + EPS) * gmlp_ref[...]
        inner_all[pl.ds(pl.multiple_of(me * rows + i * step, step), step), :] = y.astype(jnp.bfloat16)

    my_rows = pl.ds(pl.multiple_of(me * rows, rows), rows)
    inners, firsts = [], []
    for d in range(1, tp):
        peer = lax.rem(me + d, tp)
        copy = pltpu.make_async_remote_copy(
            src_ref=inner_all.at[my_rows, :],
            dst_ref=inner_all.at[my_rows, :],
            send_sem=in_send.at[d],
            recv_sem=in_recv.at[d],
            device_id={"fs": me_fs, "tp": peer},
            device_id_type=MESH,
        )
        copy.start()
        inners.append(copy)
    for d in range(1, tp):
        peer = lax.rem(me + d, tp)
        copy = pltpu.make_async_remote_copy(
            src_ref=first.at[:, pl.ds(pl.multiple_of(peer * own_cols, own_cols), own_cols)],
            dst_ref=fcols.at[my_rows, :],
            send_sem=fc_send.at[d],
            recv_sem=fc_recv.at[d],
            device_id={"fs": me_fs, "tp": peer},
            device_id_type=MESH,
        )
        copy.start()
        firsts.append(copy)
    fcols[my_rows, :] = first[:, pl.ds(pl.multiple_of(me * own_cols, own_cols), own_cols)]

    for hop in range(3, hops):
        start(UP, hop)
    settle(UP, hops - 2)
    start(DOWN, 0)
    finish(UP)
    for d in range(1, tp):
        source = pl.ds(pl.multiple_of(lax.rem(me + tp - d, tp) * rows, rows), rows)
        pltpu.make_async_remote_copy(
            src_ref=inner_all.at[source, :],
            dst_ref=inner_all.at[source, :],
            send_sem=in_send.at[d],
            recv_sem=in_recv.at[d],
            device_id={"fs": me_fs, "tp": lax.rem(me + d, tp)},
            device_id_type=MESH,
        ).wait_recv()

    tile = min(256, hid)

    @pl.loop(0, hid // tile)
    def _(j):
        h = pl.ds(pl.multiple_of(j * tile, tile), tile)
        pre = lax.dot_general(
            inner_all[...], up_full[h, :], (((1,), (1,)), ((), ())), preferred_element_type=jnp.float32
        )
        hidden[:, h] = jnp.square(jnp.maximum(pre, 0.0)).astype(jnp.bfloat16)

    sums = []

    def block(k, owner):
        c = pl.ds(pl.multiple_of(owner * cols, cols), cols)
        part = min(512, seq)

        @pl.loop(0, seq // part)
        def _(i):
            r = pl.ds(pl.multiple_of(i * part, part), part)
            blocks[k, r, :] = jnp.dot(
                hidden[r, :], down_full[:, c], preferred_element_type=jnp.float32
            ).astype(jnp.bfloat16)

        dest = owner // per
        d = lax.rem(dest - me + tp, tp)
        local = lax.rem(owner, per)
        lc = pl.ds(pl.multiple_of(local * cols, cols), cols)

        @pl.when(d == 0)
        def _():
            parts[0, :, lc] = blocks[k]

        copy = pltpu.make_async_remote_copy(
            src_ref=blocks.at[k],
            dst_ref=parts.at[d, :, lc],
            send_sem=rs_send.at[k],
            recv_sem=rs_recv.at[d * per + local],
            device_id={"fs": me_fs, "tp": dest},
            device_id_type=MESH,
        )

        @pl.when(d != 0)
        def _():
            copy.start()

        sums.append((d, copy))

    block(0, owners[0])
    k = 1
    for hop in range(1, hops):
        start(DOWN, hop)
        settle(DOWN, hop - 1)
        if hop == hops - 1:
            for side in (0, 1):
                pass
        for owner in (owners[-hop], owners[hop]):
            block(k, owner)
            k += 1
    finish(DOWN)
    block(k, owners[hops])

    for copy in started:
        copy.wait_send()
    for copy in inners:
        copy.wait_send()
    for copy in firsts:
        copy.wait()
    for d, copy in sums:
        @pl.when(d != 0)
        def _(copy=copy):
            copy.wait_send()
    for d in range(1, tp):
        for local in range(per):
            lc = pl.ds(local * cols, cols)
            pltpu.make_async_remote_copy(
                src_ref=blocks.at[0],
                dst_ref=parts.at[d, :, lc],
                send_sem=rs_send.at[0],
                recv_sem=rs_recv.at[d * per + local],
                device_id={"fs": me_fs, "tp": lax.rem(me + d, tp)},
                device_id_type=MESH,
            ).wait_recv()

    @pl.loop(0, seq // 64)
    def _(i):
        r = pl.ds(pl.multiple_of(i * 64, 64), 64)
        total = parts[0, r, :].astype(jnp.float32)
        for d in range(1, tp):
            total = total + parts[d, r, :].astype(jnp.float32)
        out_ref[r, :] = fcols[r, :].astype(jnp.float32) + total


def local(order, tokens, pool_weight, pool_scale, gain_mix, gain_mlp, w_up, w_down, gain_out):
    n, tp = lax.axis_size("fs"), lax.axis_size("tp")
    rows, width = tokens.shape
    hid, cols = w_up.shape
    seq, own = rows * tp, width // tp
    bf, f32 = jnp.bfloat16, jnp.float32
    vmem = pl.BlockSpec(memory_space=pltpu.VMEM)
    dma = pltpu.SemaphoreType.DMA
    second_sum = pl.pallas_call(
        functools.partial(kernel, n, tp, order),
        out_shape=jax.ShapeDtypeStruct((seq, own), f32),
        in_specs=[vmem] * 7,
        out_specs=vmem,
        scratch_shapes=[
            pltpu.VMEM((pool_weight.shape[0], pool_weight.shape[1] * n, pool_weight.shape[2]), bf),
            pltpu.VMEM((hid, width), bf),
            pltpu.VMEM((hid, width), bf),
            pltpu.VMEM((rows + 2 * HALO, width), f32),
            pltpu.VMEM((rows, width), bf),
            pltpu.VMEM((seq, width), bf),
            pltpu.VMEM((seq, hid), bf),
            pltpu.VMEM((seq, own), bf),
            pltpu.VMEM((n, seq, cols), bf),
            pltpu.VMEM((tp, seq, own), bf),
            pltpu.VMEM((HALO, width), bf),
            pltpu.VMEM((HALO, width), bf),
            pltpu.VMEM((2, HALO, width), bf),
            dma((12 * (n // 2),)),
            dma((12 * (n // 2),)),
            dma((tp,)),
            dma((tp,)),
            dma((tp,)),
            dma((tp,)),
            dma((2,)),
            dma((2,)),
            dma((n,)),
            dma((n,)),
        ],
        compiler_params=pltpu.CompilerParams(
            collective_id=0, has_side_effects=True, vmem_limit_bytes=63 * 1024 * 1024
        ),
    )(
        tokens, pool_weight, w_up, w_down,
        pool_scale.reshape(1, -1), gain_mix.reshape(1, -1), gain_mlp.reshape(1, -1),
    )
    squares = lax.psum(jnp.sum(second_sum * second_sum, axis=1), "tp")
    scaled = second_sum * lax.rsqrt(squares / width + EPS)[:, None] * gain_out
    return scaled.astype(jnp.bfloat16)


def grid_width(mesh):
    n = mesh.shape["fs"]
    try:
        line = mesh.devices.reshape(n, -1)[:, 0]
        nx = len({d.coords[0] for d in line})
        if n % nx == 0:
            return nx
    except AttributeError:
        pass
    return 2 if n % 2 == 0 else 1


def solution(mesh):
    order = ring_order(mesh.shape["fs"], grid_width(mesh))
    return jax.shard_map(
        functools.partial(local, order),
        mesh=mesh,
        in_specs=(
            P(("fs", "tp"), None),
            P(None, "fs", None),
            P(),
            P(),
            P(),
            P("tp", "fs"),
            P("tp", "fs"),
            P("tp"),
        ),
        out_specs=P("fs", "tp"),
        check_vma=False,
    )
```

```python
import functools

import jax
import jax.numpy as jnp
from jax import lax
from jax.experimental import pallas as pl
from jax.experimental.pallas import tpu as pltpu
from jax.sharding import PartitionSpec as P

SEQ_LEN = 1024
EPS = 1e-06
WINDOWS = (2, 4, 8, 16)
HALO = 16
MESH = pl.DeviceIdType.MESH
POOL, UP, DOWN = 0, 1, 2


def ring_order(n, nx):
    nz = n // nx
    if nx < 2 or nz < 2 or nz % 2:
        return list(range(n))
    order = []
    for z in range(nz):
        xs = list(range(1, nx))
        order += [z * nx + x for x in (xs if z % 2 == 0 else xs[::-1])]
    return order + [z * nx for z in range(nz - 1, -1, -1)]


def lookup(table, index):
    value = jnp.int32(table[0])
    for i in range(1, len(table)):
        value = jnp.where(index == i, jnp.int32(table[i]), value)
    return value


def kernel(
    n, tp, order, tok_ref, pool_ref, up_ref, down_ref, scale_ref, gmix_ref, gmlp_ref,
    gout_ref, out_ref,
    pool_full, up_full, down_full, ext, first, inner_all, hidden, fcols, blocks, parts,
    before, after, edge, total, stat, stat_out, stat_in,
    ring_send, ring_recv, in_send, in_recv, fc_send, fc_recv, halo_send, halo_recv, rs_send, rs_recv,
    pair_send, pair_recv, st_send, st_recv,
):
    rows, width = tok_ref.shape
    group = width // 4
    hid, cols = up_ref.shape
    depth = pool_ref.shape[1]
    own_cols = width // tp
    per = n // tp
    seq = rows * tp
    me_fs, me = lax.axis_index("fs"), lax.axis_index("tp")
    place_of = [order.index(i) for i in range(n)]
    place = lookup(place_of, me_fs)

    def at(offset):
        return lookup(order, lax.rem(place + offset + 2 * n, n))

    owners = {0: me_fs}
    for d in range(1, n // 2 + 1):
        owners[d] = at(d)
        owners[-d] = at(-d)
    right, left = owners[1], owners[-1]

    barrier = pltpu.get_barrier_semaphore()
    for peer in (right, left):
        pl.semaphore_signal(barrier, inc=1, device_id={"fs": peer, "tp": me}, device_id_type=MESH)
    for d in range(1, tp):
        pl.semaphore_signal(
            barrier, inc=1, device_id={"fs": me_fs, "tp": lax.rem(me + d, tp)}, device_id_type=MESH
        )
    pl.semaphore_wait(barrier, 2 + tp - 1)

    hops = n // 2
    cores = 2 if tp % 2 == 0 else 1
    core = lax.rem(me, cores)
    lanes = 2 if cols % 256 == 0 else 1
    fine = cols // lanes

    def view(stream, full, owner, piece, sub=None):
        if stream == POOL:
            ref = pool_full if full else pool_ref
            half = ref.shape[0] // (2 * cores)
            r = pl.ds(pl.multiple_of(owner * depth, depth), depth) if full else slice(None)
            return ref.at[pl.ds((core * 2 + piece) * half, half), r, :]
        ref = (up_full if full else up_ref) if stream == UP else (down_full if full else down_ref)
        half = hid // 2
        c = pl.ds(pl.multiple_of(owner * cols, cols), cols) if full else slice(None)
        if sub is not None:
            c = pl.ds(pl.multiple_of(owner * cols + sub * fine, fine), fine)
        return ref.at[pl.ds(piece * half, half), c]

    def count(side, piece):
        return hops if piece == side else hops - 1

    def slot(stream, side, piece, hop, sub):
        if sub:
            return 12 * hops + side * (lanes - 1) + sub - 1
        return ((stream * 2 + side) * 2 + piece) * hops + hop

    def subs(stream, hop):
        return range(lanes) if stream == DOWN and hop == hops - 1 and hop > 0 else (None,)

    def ring(stream, side, piece, hop, sub):
        owner = owners[-hop] if side == 0 else owners[hop]
        return pltpu.make_async_remote_copy(
            src_ref=view(stream, hop > 0, owner, piece, sub),
            dst_ref=view(stream, True, owner, piece, sub),
            send_sem=ring_send.at[slot(stream, side, piece, hop, sub)],
            recv_sem=ring_recv.at[slot(stream, side, piece, hop, sub)],
            device_id={"fs": right if side == 0 else left, "tp": me},
            device_id_type=MESH,
        )

    started = []

    def arrived(stream, side, piece, hop, sub=None):
        owner = owners[-hop - 1] if side == 0 else owners[hop + 1]
        pltpu.make_async_remote_copy(
            src_ref=view(stream, True, owner, piece, sub),
            dst_ref=view(stream, True, owner, piece, sub),
            send_sem=ring_send.at[slot(stream, side, piece, hop, sub)],
            recv_sem=ring_recv.at[slot(stream, side, piece, hop, sub)],
            device_id={"fs": right if side == 0 else left, "tp": me},
            device_id_type=MESH,
        ).wait_recv()

    def start(stream, hop, which=(0, 1)):
        for w in which:
            for side in (0, 1):
                piece = side if w == 0 else 1 - side
                if hop < count(side, piece):
                    if hop > 0:
                        arrived(stream, side, piece, hop - 1)
                    for sub in subs(stream, hop):
                        copy = ring(stream, side, piece, hop, sub)
                        copy.start()
                        started.append(copy)

    def finish(stream, sub=None):
        for side in (0, 1):
            arrived(stream, side, side, hops - 1, sub)

    def settle(stream, hop):
        if hop == hops - 2:
            for side in (0, 1):
                arrived(stream, side, 1 - side, hop)

    start(POOL, 0)
    start(UP, 0, (0,))

    step = 32 if rows % 32 == 0 else rows

    @pl.loop(0, rows // step)
    def _(i):
        r = pl.ds(pl.multiple_of(i * step, step), step)
        x = tok_ref[r, :].astype(jnp.float32)
        y = x * lax.rsqrt(jnp.mean(x * x, axis=-1, keepdims=True) + EPS) * gmix_ref[...]
        y = y.astype(jnp.bfloat16)
        ext[pl.ds(pl.multiple_of(HALO + i * step, HALO), step), :] = y.astype(jnp.float32)

    edge[0] = ext[rows : rows + HALO, :].astype(jnp.bfloat16)
    edge[1] = ext[HALO : 2 * HALO, :].astype(jnp.bfloat16)
    halos = []
    for side, (buffer, d) in enumerate(((before, 1), (after, tp - 1))):
        copy = pltpu.make_async_remote_copy(
            src_ref=edge.at[side],
            dst_ref=buffer,
            send_sem=halo_send.at[side],
            recv_sem=halo_recv.at[side],
            device_id={"fs": me_fs, "tp": lax.rem(me + d, tp)},
            device_id_type=MESH,
        )
        copy.start()
        halos.append(copy)

    start(POOL, 1)
    start(UP, 0, (1,))
    for hop in range(2, hops):
        start(POOL, hop)
    share = pl.ds(core * (pool_full.shape[0] // cores), pool_full.shape[0] // cores)
    pool_full[share, pl.ds(pl.multiple_of(me_fs * depth, depth), depth), :] = pool_ref[share, :, :]
    mine = pl.ds(pl.multiple_of(me_fs * cols, cols), cols)
    up_full[:, mine] = up_ref[...]
    down_full[:, mine] = down_ref[...]
    for copy in halos:
        copy.wait()
    offset = me * rows
    lower_open = (lax.rem(offset, SEQ_LEN) != 0).astype(jnp.float32)
    upper_open = (lax.rem(offset + rows, SEQ_LEN) != 0).astype(jnp.float32)
    ext[0:HALO, :] = before[...].astype(jnp.float32) * lower_open
    ext[rows + HALO : rows + 2 * HALO, :] = after[...].astype(jnp.float32) * upper_open
    start(UP, 1)
    settle(POOL, hops - 2)
    finish(POOL)
    if cores > 1:
        swap = pltpu.make_async_remote_copy(
            src_ref=pool_full.at[share],
            dst_ref=pool_full.at[share],
            send_sem=pair_send,
            recv_sem=pair_recv,
            device_id={"fs": me_fs, "tp": me + 1 - 2 * core},
            device_id_type=MESH,
        )
        swap.start()
        other = pl.ds((1 - core) * (pool_full.shape[0] // cores), pool_full.shape[0] // cores)
        pltpu.make_async_remote_copy(
            src_ref=pool_full.at[other],
            dst_ref=pool_full.at[other],
            send_sem=pair_send,
            recv_sem=pair_recv,
            device_id={"fs": me_fs, "tp": me + 1 - 2 * core},
            device_id_type=MESH,
        ).wait_recv()

    position = lax.rem(offset + lax.broadcasted_iota(jnp.int32, (rows, 1), 0), SEQ_LEN)
    for index, reach in enumerate(WINDOWS):
        half = reach // 2
        c = slice(index * group, (index + 1) * group)
        level = ext[:, c]
        own = level[HALO : HALO + rows]
        shift = 1
        while shift < reach:
            level = level + pltpu.roll(level, shift, 0)
            shift *= 2
        if half > 1:
            level = pltpu.roll(level, rows + 2 * HALO - (half - 1), 0)
        window = level[HALO : HALO + rows]
        counts = (jnp.minimum(position + half, SEQ_LEN) - jnp.maximum(position - half, 0)).astype(jnp.float32)
        pooled = (window / counts - own).astype(jnp.bfloat16)
        mixed = jnp.dot(pooled, pool_full[index], preferred_element_type=jnp.float32)
        first[:, c] = (tok_ref[:, c].astype(jnp.float32) + mixed * scale_ref[:, c]).astype(jnp.bfloat16)
    for hop in range(2, 3):
        if hop < hops:
            start(UP, hop)

    @pl.loop(0, rows // step)
    def _(i):
        r = pl.ds(pl.multiple_of(i * step, step), step)
        x = first[r, :].astype(jnp.float32)
        y = x * lax.rsqrt(jnp.mean(x * x, axis=-1, keepdims=True) + EPS) * gmlp_ref[...]
        inner_all[pl.ds(pl.multiple_of(me * rows + i * step, step), step), :] = y.astype(jnp.bfloat16)

    my_rows = pl.ds(pl.multiple_of(me * rows, rows), rows)
    inners, firsts = [], []
    for d in range(1, tp):
        peer = lax.rem(me + d, tp)
        copy = pltpu.make_async_remote_copy(
            src_ref=inner_all.at[my_rows, :],
            dst_ref=inner_all.at[my_rows, :],
            send_sem=in_send.at[d],
            recv_sem=in_recv.at[d],
            device_id={"fs": me_fs, "tp": peer},
            device_id_type=MESH,
        )
        copy.start()
        inners.append(copy)
    for d in range(1, tp):
        peer = lax.rem(me + d, tp)
        copy = pltpu.make_async_remote_copy(
            src_ref=first.at[:, pl.ds(pl.multiple_of(peer * own_cols, own_cols), own_cols)],
            dst_ref=fcols.at[my_rows, :],
            send_sem=fc_send.at[d],
            recv_sem=fc_recv.at[d],
            device_id={"fs": me_fs, "tp": peer},
            device_id_type=MESH,
        )
        copy.start()
        firsts.append(copy)
    fcols[my_rows, :] = first[:, pl.ds(pl.multiple_of(me * own_cols, own_cols), own_cols)]

    for hop in range(3, hops):
        start(UP, hop)
    settle(UP, hops - 2)
    start(DOWN, 0)
    finish(UP)
    for d in range(1, tp):
        source = pl.ds(pl.multiple_of(lax.rem(me + tp - d, tp) * rows, rows), rows)
        pltpu.make_async_remote_copy(
            src_ref=inner_all.at[source, :],
            dst_ref=inner_all.at[source, :],
            send_sem=in_send.at[d],
            recv_sem=in_recv.at[d],
            device_id={"fs": me_fs, "tp": lax.rem(me + d, tp)},
            device_id_type=MESH,
        ).wait_recv()

    tile = min(256, hid)

    @pl.loop(0, hid // tile)
    def _(j):
        h = pl.ds(pl.multiple_of(j * tile, tile), tile)
        pre = lax.dot_general(
            inner_all[...], up_full[h, :], (((1,), (1,)), ((), ())), preferred_element_type=jnp.float32
        )
        hidden[:, h] = jnp.square(jnp.maximum(pre, 0.0)).astype(jnp.bfloat16)

    sums = []
    part = min(512, seq)

    def block(k, owner, sub):
        c = pl.ds(pl.multiple_of(owner * cols + sub * fine, fine), fine)

        @pl.loop(0, seq // part)
        def _(i):
            r = pl.ds(pl.multiple_of(i * part, part), part)
            blocks[k, sub, r, :] = jnp.dot(
                hidden[r, :], down_full[:, c], preferred_element_type=jnp.float32
            ).astype(jnp.bfloat16)

        dest = owner // per
        d = lax.rem(dest - me + tp, tp)
        local = lax.rem(owner, per)
        copy = pltpu.make_async_remote_copy(
            src_ref=blocks.at[k, sub],
            dst_ref=parts.at[d, local, sub],
            send_sem=rs_send.at[k * lanes + sub],
            recv_sem=rs_recv.at[(d * per + local) * lanes + sub],
            device_id={"fs": me_fs, "tp": dest},
            device_id_type=MESH,
        )

        @pl.when(d == 0)
        def _():
            parts[0, local, sub] = blocks[k, sub]

        @pl.when(d != 0)
        def _():
            copy.start()

        sums.append((d, copy))

    def add_up(local, sub):
        for d in range(1, tp):
            pltpu.make_async_remote_copy(
                src_ref=blocks.at[0, sub],
                dst_ref=parts.at[d, local, sub],
                send_sem=rs_send.at[0],
                recv_sem=rs_recv.at[(d * per + local) * lanes + sub],
                device_id={"fs": me_fs, "tp": lax.rem(me + d, tp)},
                device_id_type=MESH,
            ).wait_recv()
        c = pl.ds(pl.multiple_of(local * cols + sub * fine, fine), fine)

        @pl.loop(0, seq // 128)
        def _(i):
            r = pl.ds(pl.multiple_of(i * 128, 128), 128)
            value = parts[0, local, sub, r, :].astype(jnp.float32)
            for d in range(1, tp):
                value = value + parts[d, local, sub, r, :].astype(jnp.float32)
            value = value + fcols[r, c].astype(jnp.float32)
            total[r, c] = value
            square = value * value
            lump = square[:, 0:128]
            for j in range(1, fine // 128):
                lump = lump + square[:, j * 128 : (j + 1) * 128]
            stat[r, :] = stat[r, :] + lump

    for sub in range(lanes):
        block(0, owners[0], sub)
    stat[...] = jnp.zeros_like(stat)
    k = 1
    for hop in range(1, hops):
        start(DOWN, hop)
        settle(DOWN, hop - 1)
        for owner in (owners[-hop], owners[hop]):
            for sub in range(lanes):
                block(k, owner, sub)
            k += 1
    for copy in firsts:
        copy.wait()
    last = lax.rem(owners[hops], per)
    for j in range(1, per):
        for sub in range(lanes):
            add_up(lax.rem(last + j, per), sub)
    for sub in range(lanes):
        finish(DOWN, sub)
        block(k, owners[hops], sub)
    for sub in range(lanes):
        add_up(last, sub)

    turned = jnp.transpose(stat[...])
    stat_out[...] = jnp.broadcast_to(jnp.sum(turned, axis=0, keepdims=True), stat_out.shape)
    stats = []
    for d in range(1, tp):
        copy = pltpu.make_async_remote_copy(
            src_ref=stat_out,
            dst_ref=stat_in.at[d],
            send_sem=st_send.at[d],
            recv_sem=st_recv.at[d],
            device_id={"fs": me_fs, "tp": lax.rem(me + d, tp)},
            device_id_type=MESH,
        )
        copy.start()
        stats.append(copy)
    for copy in started:
        copy.wait_send()
    for copy in inners:
        copy.wait_send()
    if cores > 1:
        swap.wait_send()
    for d, copy in sums:
        @pl.when(d != 0)
        def _(copy=copy):
            copy.wait_send()
    for copy in stats:
        copy.wait()
    squares = stat_out[...]
    for d in range(1, tp):
        squares = squares + stat_in[d]
    factor = lax.rsqrt(squares / width + EPS)
    stat[...] = jnp.transpose(jnp.broadcast_to(factor[0:1], (128, seq)))

    @pl.loop(0, seq // 128)
    def _(i):
        r = pl.ds(pl.multiple_of(i * 128, 128), 128)
        out_ref[r, :] = (total[r, :] * stat[r, 0:1] * gout_ref[...]).astype(jnp.bfloat16)


def local(order, tokens, pool_weight, pool_scale, gain_mix, gain_mlp, w_up, w_down, gain_out):
    n, tp = lax.axis_size("fs"), lax.axis_size("tp")
    rows, width = tokens.shape
    hid, cols = w_up.shape
    seq, own = rows * tp, width // tp
    bf, f32 = jnp.bfloat16, jnp.float32
    vmem = pl.BlockSpec(memory_space=pltpu.VMEM)
    dma = pltpu.SemaphoreType.DMA
    lanes = 2 if cols % 256 == 0 else 1
    return pl.pallas_call(
        functools.partial(kernel, n, tp, order),
        out_shape=jax.ShapeDtypeStruct((seq, own), bf),
        in_specs=[vmem] * 8,
        out_specs=vmem,
        scratch_shapes=[
            pltpu.VMEM((pool_weight.shape[0], pool_weight.shape[1] * n, pool_weight.shape[2]), bf),
            pltpu.VMEM((hid, width), bf),
            pltpu.VMEM((hid, width), bf),
            pltpu.VMEM((rows + 2 * HALO, width), f32),
            pltpu.VMEM((rows, width), bf),
            pltpu.VMEM((seq, width), bf),
            pltpu.VMEM((seq, hid), bf),
            pltpu.VMEM((seq, own), bf),
            pltpu.VMEM((n, lanes, seq, cols // lanes), bf),
            pltpu.VMEM((tp, n // tp, lanes, seq, cols // lanes), bf),
            pltpu.VMEM((HALO, width), bf),
            pltpu.VMEM((HALO, width), bf),
            pltpu.VMEM((2, HALO, width), bf),
            pltpu.VMEM((seq, own), f32),
            pltpu.VMEM((seq, 128), f32),
            pltpu.VMEM((8, seq), f32),
            pltpu.VMEM((tp, 8, seq), f32),
            dma((12 * (n // 2) + 2 * lanes,)),
            dma((12 * (n // 2) + 2 * lanes,)),
            dma((tp,)),
            dma((tp,)),
            dma((tp,)),
            dma((tp,)),
            dma((2,)),
            dma((2,)),
            dma((n * lanes,)),
            dma((n * lanes,)),
            dma,
            dma,
            dma((tp,)),
            dma((tp,)),
        ],
        compiler_params=pltpu.CompilerParams(
            collective_id=0, has_side_effects=True, vmem_limit_bytes=63 * 1024 * 1024
        ),
    )(
        tokens, pool_weight, w_up, w_down,
        pool_scale.reshape(1, -1), gain_mix.reshape(1, -1), gain_mlp.reshape(1, -1),
        gain_out.reshape(1, -1),
    )


def grid_width(mesh):
    n = mesh.shape["fs"]
    try:
        line = mesh.devices.reshape(n, -1)[:, 0]
        nx = len({d.coords[0] for d in line})
        if n % nx == 0:
            return nx
    except AttributeError:
        pass
    return 2 if n % 2 == 0 else 1


def solution(mesh):
    order = ring_order(mesh.shape["fs"], grid_width(mesh))
    return jax.shard_map(
        functools.partial(local, order),
        mesh=mesh,
        in_specs=(
            P(("fs", "tp"), None),
            P(None, "fs", None),
            P(),
            P(),
            P(),
            P("tp", "fs"),
            P("tp", "fs"),
            P("tp"),
        ),
        out_specs=P("fs", "tp"),
        check_vma=False,
    )
```
